512 devices in a mesh: grp: 2 (over y), sp: 16 (over z), tp: 16 (over x, core).
Axes of the slice: x: 8, y: 2, z: 16, core: 2. Of those that a mesh axis runs over, the one named last changes fastest.
The devices are a block of a 8x16x16 slice.
Arguments:
- target: bfloat16 [4096, 2048], P(('grp', 'sp', 'tp')), parts along dimension 0, may hold values from -6 to 6
- source: bfloat16 [32768, 2048], P(('grp', 'sp', 'tp')), parts along dimension 0, may hold values from -6 to 6
- norm_gain: float32 [2048], replicated, may hold values from 0.1 to 1.9
- query_weight: bfloat16 [2048, 2048], P(None, 'tp'), may hold values from -0.125 to 0.125
- key_weight: bfloat16 [2048, 256], replicated, may hold values from -0.125 to 0.125
- value_weight: bfloat16 [2048, 256], replicated, may hold values from -0.125 to 0.125
- output_weight: bfloat16 [2048, 2048], P('tp'), may hold values from -0.125 to 0.125
- saved_out: bfloat16 [4096, 2048], P(('grp', 'sp'), 'tp'), parts along dimension 0, may hold values from -3 to 3
- log_shift: float32 [16, 4096], P('tp', ('grp', 'sp')), parts along dimension 1, may hold values from 0 to 2
- out_grad: bfloat16 [4096, 2048], P(('grp', 'sp', 'tp')), parts along dimension 0, may hold values from -48 to 48
Outputs:
- target_grad: float32 [4096, 2048], P(('grp', 'sp', 'tp')), parts along dimension 0
- source_grad: float32 [32768, 2048], P(('grp', 'sp', 'tp')), parts along dimension 0
- query_weight_grad: float32 [4096, 2048], P(('grp', 'sp'), 'tp'), parts along dimension 0
The draws below stay inside these ranges and needn't reach their ends.
There are 2 independent parts, one for each index of `grp`. The reference program is written for one: setup_inputs(seed, part) draws one part's arguments, and reference() takes and returns one part's arrays. A program takes and returns all parts, laid end to end along the dimension named above; an argument that names none is the same for every part. Nothing has to cross between parts.
All inputs are finite; a program needn't handle non-finite values.
Results may differ from the reference program's by a relative error of at most 0.02.
Values may be sent and summed in bfloat16 or wider, within the bound.
A program may use at most 64 MiB of HBM per device.

```python
import jax
import jax.numpy as jnp
from jax import lax

D = 2048
HEADS = 16
HEAD_DIM = 128
KV_HEADS = 2
SRC = 16384
TGT = 2048


def shard_levels(stream_key, extent, shards, low, top_value):
    def one(axis_at, shards_of):
        steps = jax.random.uniform(jax.random.fold_in(jax.random.fold_in(stream_key, 6), axis_at), (shards_of,), jnp.float32, low / len(shards), top_value / len(shards))
        return jnp.repeat(jnp.exp(steps), extent[axis_at] // shards_of).reshape((-1,) + (1,) * (len(extent) - axis_at - 1))

    gain = one(*shards[0])
    for cut in shards[1:]:
        gain = gain * one(*cut)
    return gain


def centred(rng, shape, spread, reach, pieces=(), kind=jnp.bfloat16):
    loudness = shard_levels(rng, shape, pieces, -0.22, 0.18) if pieces else 1.0
    entries = jax.random.normal(rng, shape, jnp.float32) * spread * loudness
    return jnp.minimum(jnp.maximum(entries, -reach), reach).astype(kind)


def setup_inputs(seed: int = 0, part: int = 0) -> dict:
    splits = jax.random.split(jax.random.key(seed), 11)
    part_splits = jax.random.split(jax.random.fold_in(splits[10], part), 11)
    target = centred(part_splits[0], (TGT, D), 1.0, 6.0, ((0, 256),))
    source = centred(part_splits[1], (SRC, D), 1.0, 6.0, ((0, 256),))
    norm_gain = jnp.clip(1.0 + 0.18 * jax.random.normal(splits[2], (D,), jnp.float32), 0.1, 1.9)
    query_weight = centred(splits[3], (D, HEADS * HEAD_DIM), D ** -0.5, 0.125, ((1, 16),))
    key_weight = centred(splits[4], (D, KV_HEADS * HEAD_DIM), D ** -0.5, 0.125)
    value_weight = centred(splits[5], (D, KV_HEADS * HEAD_DIM), D ** -0.5, 0.125)
    output_weight = centred(splits[6], (HEADS * HEAD_DIM, D), (HEADS * HEAD_DIM) ** -0.5, 0.125, ((0, 16),))
    saved_out = centred(part_splits[7], (TGT, HEADS * HEAD_DIM), 0.5, 3.0, ((0, 16), (1, 16)))
    log_shift = jnp.clip(2.0 * jax.random.uniform(part_splits[8], (HEADS, TGT), jnp.float32) ** shard_levels(part_splits[8], (HEADS, TGT), ((0, 16), (1, 16)), -0.2, 0.2), 0.0, 2.0)
    out_grad = centred(part_splits[9], (TGT, D), 8.0, 48.0, ((0, 256),))
    return dict(target=target, source=source, norm_gain=norm_gain, query_weight=query_weight, key_weight=key_weight, value_weight=value_weight, output_weight=output_weight, saved_out=saved_out, log_shift=log_shift, out_grad=out_grad)


def reference(target, source, norm_gain, query_weight, key_weight, value_weight, output_weight, saved_out, log_shift, out_grad):
    group_size = HEADS // KV_HEADS
    factor = HEAD_DIM ** (-0.5)
    offset = jnp.log(jnp.float32(SRC))
    target_wide = target.astype(jnp.float32)
    root_mean = jnp.sqrt(lax.optimization_barrier(jnp.mean(target_wide * target_wide, axis=1, keepdims=True)) + 1e-06)
    normed = (target_wide / root_mean * norm_gain).astype(jnp.bfloat16)
    queries = jnp.dot(normed, query_weight, preferred_element_type=jnp.float32).astype(jnp.bfloat16)
    key_rows = jnp.dot(source, key_weight, preferred_element_type=jnp.float32).astype(jnp.bfloat16)
    values = jnp.dot(source, value_weight, preferred_element_type=jnp.float32).astype(jnp.bfloat16)
    out_back = jnp.dot(out_grad, output_weight.T, preferred_element_type=jnp.float32).astype(jnp.bfloat16)
    products = out_back.astype(jnp.float32) * saved_out.astype(jnp.float32)
    drop_term = lax.optimization_barrier(jnp.sum(products.reshape(TGT, HEADS, HEAD_DIM), axis=2))

    def one_head(head_id):
        pair_index = head_id // group_size
        query_head = lax.dynamic_slice_in_dim(queries, head_id * HEAD_DIM, HEAD_DIM, 1)
        back_head = lax.dynamic_slice_in_dim(out_back, head_id * HEAD_DIM, HEAD_DIM, 1)
        key_head = lax.dynamic_slice_in_dim(key_rows, pair_index * HEAD_DIM, HEAD_DIM, 1)
        value_head = lax.dynamic_slice_in_dim(values, pair_index * HEAD_DIM, HEAD_DIM, 1)
        shift_row = lax.dynamic_index_in_dim(log_shift, head_id, 0, keepdims=False)
        drop_row = lax.dynamic_index_in_dim(drop_term, head_id, 1, keepdims=False)
        scores = jnp.dot(query_head, key_head.T, preferred_element_type=jnp.float32) * factor
        prob = jnp.exp(scores - shift_row[:, None] - offset)
        prob_grad = jnp.dot(back_head, value_head.T, preferred_element_type=jnp.float32)
        score_grad = (prob * (prob_grad - drop_row[:, None]) * factor).astype(jnp.bfloat16)
        prob_low = prob.astype(jnp.bfloat16)
        query_part = jnp.dot(score_grad, key_head, preferred_element_type=jnp.float32)
        key_part = jnp.dot(score_grad.T, query_head, preferred_element_type=jnp.float32)
        value_part = jnp.dot(prob_low.T, back_head, preferred_element_type=jnp.float32)
        return (query_part, key_part, value_part)
    head_ids = jnp.arange(HEADS, dtype=jnp.int32)
    query_all, key_all, value_all = lax.map(one_head, head_ids)
    query_grad = jnp.transpose(query_all, (1, 0, 2)).reshape(TGT, HEADS * HEAD_DIM).astype(jnp.bfloat16)
    key_sum = lax.optimization_barrier(jnp.sum(key_all.reshape(KV_HEADS, group_size, SRC, HEAD_DIM), axis=1))
    value_sum = lax.optimization_barrier(jnp.sum(value_all.reshape(KV_HEADS, group_size, SRC, HEAD_DIM), axis=1))
    key_grad = jnp.transpose(key_sum, (1, 0, 2)).reshape(SRC, KV_HEADS * HEAD_DIM).astype(jnp.bfloat16)
    value_grad = jnp.transpose(value_sum, (1, 0, 2)).reshape(SRC, KV_HEADS * HEAD_DIM).astype(jnp.bfloat16)
    source_grad = jnp.dot(key_grad, key_weight.T, preferred_element_type=jnp.float32) + jnp.dot(value_grad, value_weight.T, preferred_element_type=jnp.float32)
    normed_grad = jnp.dot(query_grad, query_weight.T, preferred_element_type=jnp.float32)
    scaled_grad = normed_grad * norm_gain
    target_grad = scaled_grad / root_mean - target_wide * lax.optimization_barrier(jnp.mean(scaled_grad * target_wide, axis=1, keepdims=True)) / root_mean ** 3
    query_weight_grad = jnp.dot(normed.T, query_grad, preferred_element_type=jnp.float32)
    return (target_grad, source_grad, query_weight_grad)
```

```python
import functools
import math

import jax
import jax.numpy as jnp
from jax import lax
from jax.experimental import pallas as pl
from jax.experimental.pallas import tpu as pltpu
from jax.sharding import PartitionSpec as P

HEAD_DIM = 128
KV_HEADS = 2
A_SUBS = 4
C_SUBS = 2
R_SUBS = 2
TILE = 512
FIRST = 3
LOG2E = math.log2(math.e)
F32, BF16 = jnp.float32, jnp.bfloat16
NT = (((1,), (1,)), ((), ()))


def dot(a, b, dims=(((1,), (0,)), ((), ()))):
    return lax.dot_general(a, b, dims, preferred_element_type=F32)


class Sems:
    def __init__(self, ref, size):
        self.ref, self.size, self.names = ref, size, {}

    def __getitem__(self, name):
        index = self.names.setdefault(name, len(self.names))
        assert index < self.size, index
        return self.ref.at[index]


def kernel(sizes, *refs):
    n, m, rows, srows, width = sizes
    chips, half_n, half_x = m // 2, n // 2, m // 4
    tgt, src = rows * m, srows * m
    (t_h, s_h, gain_h, wq_h, kw_h, vw_h, wo_h, saved_h, shift_h, og_h) = refs[:10]
    (tg_h, sg_h, wg_h) = refs[10:13]
    (
        t_v, s_v, gain_v, wq2, kw_v, vw_v, wo2, saved2, shift2,
        kinds, rows_all, rows_mat, nrm_mat, kvs, kv_all, k_t, blk, stg, stat_s, stat,
        acc, dqp, gp, d_snd, d_raw, d_sum, g_snd, g_raw, g_sum,
        pk_s, pk_r, ek_s, ek_r, dq_s, dq_r, f_s, f_r, tg_v, sg_v, wg_v,
        load_ref, send_ref, recv_ref, c_send, c_recv, st_send,
    ) = refs[13:]
    tp, sp = lax.axis_index("tp"), lax.axis_index("sp")
    x, c = tp // 2, tp % 2
    mate = x * 2 + 1 - c

    def chip(o):
        return (x + o + chips) % chips

    def ring(o):
        return (sp + o + n) % n

    loads, sends, recvs = Sems(load_ref, 16), Sems(send_ref, 400), Sems(recv_ref, 400)
    started = []

    def load(source, target, name):
        copy = pltpu.make_async_copy(source, target, loads[name])
        copy.start()
        return copy

    def send(source, target, name, device, key=None):
        copy = pltpu.make_async_remote_copy(
            src_ref=source, dst_ref=target, send_sem=sends[key or name + (len(started),)],
            recv_sem=recvs[name], device_id=device, device_id_type=pl.DeviceIdType.MESH,
        )
        copy.start()
        started.append(copy)

    def arrive(target, sem):
        pltpu.make_async_remote_copy(
            src_ref=target, dst_ref=target, send_sem=send_ref.at[0], recv_sem=sem,
            device_id={"tp": mate}, device_id_type=pl.DeviceIdType.MESH,
        ).wait_recv()

    get_t = load(t_h, t_v, "t")
    get_gain = load(gain_h, gain_v, "gain")
    get_og = load(og_h, kinds.at[1], "og")
    get_s = load(s_h, s_v, "s")
    get_kw = load(kw_h, kw_v, "kw")
    get_vw = load(vw_h, vw_v, "vw")
    get_wq = load(wq_h, wq2.at[:, 0:HEAD_DIM], "wq")
    get_wo = load(wo_h, wo2.at[0:HEAD_DIM], "wo")
    get_saved = load(saved_h, saved2.at[0], "saved")
    get_shift = load(shift_h, shift2.at[0], "shift")

    peers = [{"tp": chip(o) * 2 + c} for o in range(1, chips)]
    peers += [{"tp": chip(o) * 2 + 1 - c} for o in (-1, 0, 1)]
    peers += [{"sp": ring(o)} for o in (-2, -1, 1, 2)]
    peers += [{"sp": ring(o), "tp": mate} for o in (-1, 1)]
    barrier = pltpu.get_barrier_semaphore()
    for peer in peers:
        pl.semaphore_signal(barrier, inc=1, device_id=peer, device_id_type=pl.DeviceIdType.MESH)

    get_t.wait()
    get_gain.wait()
    wide = t_v[...].astype(F32)
    root = jnp.sqrt(jnp.mean(wide * wide, axis=1, keepdims=True) + 1e-06)
    kinds[0] = (wide / root * gain_v[...]).astype(BF16)
    get_og.wait()
    rows_all[tp] = kinds[c]
    pl.semaphore_wait(barrier, len(peers))

    part = width // A_SUBS
    cuts = [pl.ds(i * part, part) for i in range(A_SUBS)]
    for i, cut in enumerate(cuts):
        for way in (1, -1):
            if half_x == 0 or (half_x == 1 and (i < A_SUBS // 2) != (way == 1)):
                continue
            for k in (0, 1):
                copy = pltpu.make_async_remote_copy(
                    src_ref=kinds.at[k, :, cut], dst_ref=rows_all.at[tp, :, cut],
                    send_sem=sends["a1", i, way, k],
                    recv_sem=recv_ref.at[((way + 1) // 2 * A_SUBS + i) * 2 + c],
                    device_id={"tp": chip(way) * 2 + k}, device_id_type=pl.DeviceIdType.MESH,
                )
                copy.start()
                started.append(copy)
    for index in range(A_SUBS * 4):
        recvs["first", index]
    send(kinds.at[1 - c], rows_all.at[tp], ("mate_rows",), {"tp": mate})
    send(wq_h, wq2.at[:, HEAD_DIM : 2 * HEAD_DIM], ("wq",), {"tp": mate})
    send(wo_h, wo2.at[HEAD_DIM : 2 * HEAD_DIM], ("wo",), {"tp": mate})
    send(saved_h, saved2.at[1], ("saved",), {"tp": mate})
    send(shift_h, shift2.at[1], ("shift",), {"tp": mate})

    get_s.wait()
    get_kw.wait()
    get_vw.wait()
    keys = dot(s_v[...], kw_v[...]).astype(BF16)
    values = dot(s_v[...], vw_v[...]).astype(BF16)
    for g in range(KV_HEADS):
        piece = slice(g * HEAD_DIM, (g + 1) * HEAD_DIM)
        kvs[g, :, 0:HEAD_DIM] = keys[:, piece]
        kvs[g, :, HEAD_DIM:] = values[:, piece]

    def send_kv(o):
        to = chip(o)
        send(kvs.at[to // half_x], kv_all.at[tp], ("kv", o), {"tp": to * 2 + c})

    def a_arrive(hop, way, i):
        if hop == 1:
            for k in (0, 1):
                slot = chip(-way) * 2 + k
                arrive(
                    rows_all.at[slot, :, cuts[i]],
                    recv_ref.at[((way + 1) // 2 * A_SUBS + i) * 2 + k],
                )
        else:
            slot = chip(-way * hop) * 2
            arrive(rows_all.at[pl.ds(slot, 2), :, cuts[i]], recvs["a", hop, way, i])

    def a_on(hop, way, i):
        return hop < half_x_ring or (hop == half_x_ring and (i < A_SUBS // 2) == (way == 1))

    half_x_ring = chips // 2
    near = [o for k in range(1, half_x_ring + 1) for o in (k, -k)][: chips - 1]
    offsets = near[::-1]
    for hop in range(1, half_x_ring + 1):
        for i in range(A_SUBS):
            for way in (1, -1):
                if not a_on(hop, way, i):
                    continue
                a_arrive(hop, way, i)
                if a_on(hop + 1, way, i):
                    slot = chip(-way * hop) * 2
                    piece = rows_all.at[pl.ds(slot, 2), :, cuts[i]]
                    send(piece, piece, ("a", hop + 1, way, i), {"tp": chip(way) * 2 + c})
        if hop >= half_x_ring - 1:
            while offsets and (hop >= half_x_ring - 1):
                send_kv(offsets.pop(0))
        if hop == 1:
            kv_all[tp] = kvs[x // half_x]
            blk[:, 0:tgt, HEAD_DIM:] = jnp.zeros((n, tgt, HEAD_DIM), BF16)
            blk[:, tgt:, 0:HEAD_DIM] = jnp.zeros((n, tgt, HEAD_DIM), BF16)
            acc[...] = jnp.zeros(acc.shape, F32)
    arrive(rows_all.at[tp], recvs["mate_rows",])
    rows_mat[...] = rows_all[...].astype(F32).reshape(tgt, width).astype(BF16)
    get_wq.wait()
    get_wo.wait()
    get_saved.wait()
    get_shift.wait()
    for name, target in (
        ("wq", wq2.at[:, HEAD_DIM : 2 * HEAD_DIM]), ("wo", wo2.at[HEAD_DIM : 2 * HEAD_DIM]),
        ("saved", saved2.at[1]), ("shift", shift2.at[1]),
    ):
        arrive(target, recvs[name,])

    offset = math.log(n * src)

    @pl.when(c == 0)
    def _():
        both = dot(rows_mat[...], wq2[...]).astype(BF16)
        stg[0] = both[:, 0:HEAD_DIM]
        stg[1] = both[:, HEAD_DIM:]

    @pl.when(c == 1)
    def _():
        both = dot(rows_mat[...], wo2[...], NT).astype(BF16)
        stg[0] = both[:, 0:HEAD_DIM]
        stg[1] = both[:, HEAD_DIM:]
        for k in (0, 1):
            product = stg[k].astype(F32) * saved2[k].astype(F32)
            stat_s[k, 0:1, :] = (shift2[k] + offset) * LOG2E
            stat_s[k, 1:2, :] = jnp.sum(product.T, axis=0, keepdims=True)
        stat[sp] = stat_s[0]

    piece_rows = tgt // C_SUBS

    def c_piece(b, kind, i):
        return blk.at[
            b, pl.ds(kind * tgt + i * piece_rows, piece_rows), pl.ds(kind * HEAD_DIM, HEAD_DIM)
        ]

    c_copies, st_copies = [], []
    mine = pl.multiple_of(c * tgt, tgt)
    lane = pl.multiple_of(c * HEAD_DIM, HEAD_DIM)
    for i in range(C_SUBS):
        for way in (1, -1):
            for k in (0, 1):
                copy = pltpu.make_async_remote_copy(
                    src_ref=stg.at[k, pl.ds(i * piece_rows, piece_rows)],
                    dst_ref=blk.at[
                        sp,
                        pl.ds(pl.multiple_of(mine + i * piece_rows, piece_rows), piece_rows),
                        pl.ds(lane, HEAD_DIM),
                    ],
                    send_sem=c_send.at[(way + 1) // 2, i, k],
                    recv_sem=c_recv.at[(way + 1) // 2, 1, c, i],
                    device_id={"sp": ring(way), "tp": tp if k == 0 else mate},
                    device_id_type=pl.DeviceIdType.MESH,
                )
                copy.start()
                c_copies.append(copy)
    for way in (1, -1):
        for k in (0, 1):
            st_copies.append(
                pltpu.make_async_remote_copy(
                    src_ref=stat_s.at[k], dst_ref=stat.at[sp],
                    send_sem=st_send.at[(way + 1) // 2, k],
                    recv_sem=recvs["stat", way, 1],
                    device_id={"sp": ring(way), "tp": tp if k == 0 else mate},
                    device_id_type=pl.DeviceIdType.MESH,
                )
            )
    mate_stat = pltpu.make_async_remote_copy(
        src_ref=stat_s.at[1], dst_ref=stat.at[sp], send_sem=st_send.at[2, 0],
        recv_sem=recvs["mate_stat",], device_id={"tp": mate}, device_id_type=pl.DeviceIdType.MESH,
    )
    mate_rows = pltpu.make_async_remote_copy(
        src_ref=rows_mat, dst_ref=nrm_mat, send_sem=st_send.at[2, 1],
        recv_sem=recvs["nrm",], device_id={"tp": mate}, device_id_type=pl.DeviceIdType.MESH,
    )
    send(
        stg.at[1], blk.at[sp, pl.ds(mine, tgt), pl.ds(lane, HEAD_DIM)], ("mate_block",),
        {"tp": mate},
    )
    blk[sp, pl.ds(mine, tgt), pl.ds(lane, HEAD_DIM)] = stg[0]

    @pl.when(c == 1)
    def _():
        for copy in st_copies:
            copy.start()
        mate_stat.start()

    @pl.when(c == 0)
    def _():
        mate_rows.start()
        nrm_mat[...] = rows_mat[...]

    def c_on(hop, way, kind):
        return hop < half_n or (hop == half_n and (kind == 1) == (way == -1))

    def c_hop(hop):
        for i in range(C_SUBS):
            for kind in (0, 1):
                for way in (1, -1):
                    if not c_on(hop, way, kind):
                        continue
                    piece = c_piece(ring(-way * hop), kind, i)
                    arrive(piece, c_recv.at[(way + 1) // 2, hop, kind, i])
                    if c_on(hop + 1, way, kind):
                        copy = pltpu.make_async_remote_copy(
                            src_ref=piece, dst_ref=piece,
                            send_sem=sends["c", hop, kind, way, i],
                            recv_sem=c_recv.at[(way + 1) // 2, hop + 1, kind, i],
                            device_id={"sp": ring(way)}, device_id_type=pl.DeviceIdType.MESH,
                        )
                        copy.start()
                        started.append(copy)
        for way in (1, -1):
            if c_on(hop, way, 0):
                piece = stat.at[ring(-way * hop)]
                arrive(piece, recvs["stat", way, hop])
                if c_on(hop + 1, way, 0):
                    send(piece, piece, ("stat", way, hop + 1), {"sp": ring(way)})

    def kv_ready():
        for o in [0] + near:
            slot = kv_all.at[chip(-o) * 2 + c]
            if o != 0:
                arrive(slot, recvs["kv", o])
            send(slot, slot, ("kv_mate", o), {"tp": mate})
        for o in [0] + near:
            arrive(kv_all.at[chip(-o) * 2 + 1 - c], recvs["kv_mate", o])
        k_t[...] = kv_all[:, :, 0:HEAD_DIM].reshape(src, HEAD_DIM).T

        @pl.when(c == 0)
        def _():
            arrive(c_own(1), recvs["mate_block",])
            arrive(stat.at[sp], recvs["mate_stat",])

        @pl.when(c == 1)
        def _():
            arrive(c_own(0), recvs["mate_block",])

    def c_own(kind):
        return blk.at[sp, kind * tgt : (kind + 1) * tgt, kind * HEAD_DIM : (kind + 1) * HEAD_DIM]

    factor = HEAD_DIM ** (-0.5)
    tile = min(TILE, src)
    step = tile // srows

    def attend(index, carry):
        away = (index + 1) // 2 * (1 - 2 * (index % 2))
        b = (sp + away + n) % n
        block = blk[b]
        stats = stat[b]
        total = jnp.zeros((HEAD_DIM, tgt), F32)
        for at in range(0, m, step):
            kv = kv_all[at : at + step].reshape(tile, 2 * HEAD_DIM)
            both = dot(kv, block, NT)
            prob = jnp.exp2(both[:, 0:tgt] * (factor * LOG2E) - stats[0:1])
            grad = (prob * (both[:, tgt:] - stats[1:2])).astype(BF16)
            pair = jnp.concatenate([grad, prob.astype(BF16)], axis=1)
            added = dot(pair, block).reshape(step // 2, 2, srows, 2 * HEAD_DIM)
            acc[at // 2 : (at + step) // 2] += added
            total += dot(k_t[:, at * srows : at * srows + tile], grad)
        dqp[b] = total
        return carry

    done = 0
    for hop in range(1, half_n + 1):
        c_hop(hop)
        if hop == min(FIRST, half_n):
            kv_ready()
        if hop >= min(FIRST, half_n):
            have = n if hop == half_n else 1 + 2 * hop
            upto = have if hop == half_n else min(have, done + 4)
            lax.fori_loop(done, upto, attend, 0)
            done = upto

    def ring_sum(name, own, snd, raw, total, between):
        chunk = HEAD_DIM // R_SUBS
        limits = (half_n, half_n - 1)
        order = []
        for d in range(half_n, 0, -1):
            for side in (0, 1):
                if d <= limits[side]:
                    order.append((side, d))

        def block(side, d):
            return ring(-d if side == 0 else d)

        def put(side, d, i):
            cut = pl.ds(i * chunk, chunk)
            back = -1 if side == 0 else 1
            into = raw if d % 2 else total
            send(
                snd.at[side, d, cut], into.at[side, d, cut], (name, side, d, i),
                {"sp": ring(back if d % 2 else 2 * back)},
            )

        def term(side, d, i, value):
            cut = pl.ds(i * chunk, chunk)
            if d + 1 <= limits[side]:
                arrive(raw.at[side, d + 1, cut], recvs[name, side, d + 1, i])
                value += raw[side, d + 1, cut].astype(F32)
            if d + 2 <= limits[side]:
                arrive(total.at[side, d + 2, cut], recvs[name, side, d + 2, i])
                value += total[side, d + 2, cut].astype(F32)
            return value

        for side, d in order:
            if d % 2 or d == half_n:
                snd[side, d] = own(block(side, d), slice(None)).astype(BF16)
                for i in range(R_SUBS):
                    put(side, d, i)
        between(0)
        for stage, d in enumerate(range(half_n - 2, 0, -2)):
            if stage:
                between(stage)
            for i in range(R_SUBS):
                for side in (0, 1):
                    cut = pl.ds(i * chunk, chunk)
                    snd[side, d, cut] = term(side, d, i, own(block(side, d), cut)).astype(BF16)
                    put(side, d, i)
        for stage in range(max(1, half_n // 2 - 1), 4):
            between(stage)
        parts = []
        for i in range(R_SUBS):
            value = own(sp, pl.ds(i * chunk, chunk))
            for side in (0, 1):
                value = term(side, 0, i, value)
            parts.append(value)
        return jnp.concatenate(parts, axis=0)

    def own_dq(b, cut):
        return dqp[b, cut]

    def kv_pair(stage):
        if stage == 0:
            pk_s[...] = acc[:, 1 - c].astype(BF16)
            send(pk_s, pk_r, ("pk",), {"tp": mate})
        if stage == 1:
            arrive(pk_r, recvs["pk",])
            ek_s[...] = (acc[:, c] + pk_r[...].astype(F32)).astype(BF16)
            for o in near[::-1]:
                send(ek_s.at[chip(o)], ek_r.at[x], ("ek", o), {"tp": chip(o) * 2 + c})
            ek_r[x] = ek_s[x]

    dq_t = (ring_sum("d", own_dq, d_snd, d_raw, d_sum, kv_pair) * factor).astype(BF16)

    dq_rows = dq_t.astype(F32).T.reshape(chips, 2, rows, HEAD_DIM)
    dq_s[0] = dq_rows[:, 0].astype(BF16)
    dq_s[1] = dq_rows[:, 1].astype(BF16)
    send(dq_s.at[1 - c], dq_r, ("dq",), {"tp": mate})

    @pl.when(c == 1)
    def _():
        arrive(nrm_mat, recvs["nrm",])

    shares = dot(dq_t, nrm_mat[...])
    cols = width // n
    for b in range(n):
        gp[b] = shares[:, b * cols : (b + 1) * cols]

    def row_share():
        arrive(dq_r, recvs["dq",])
        left = dq_s[c].astype(F32).reshape(chips * rows, HEAD_DIM).astype(BF16)
        right = dq_r[...].astype(F32).reshape(chips * rows, HEAD_DIM).astype(BF16)
        share = dot(jnp.concatenate([left, right], axis=1), wq2[...], NT)
        f_s[...] = share.reshape(chips, rows, width).astype(BF16)
        for o in near[::-1]:
            send(f_s.at[chip(o)], f_r.at[x], ("f", o), {"tp": chip(o) * 2 + c})
        f_r[x] = f_s[x]

    put_sg = pltpu.make_async_copy(sg_v, sg_h, loads["sg"])
    put_tg = pltpu.make_async_copy(tg_v, tg_h, loads["tg"])
    put_wg = pltpu.make_async_copy(wg_v, wg_h, loads["wg"])

    def source_out():
        for o in near:
            arrive(ek_r.at[chip(-o)], recvs["ek", o])
        sums = [
            jnp.sum(ek_r[g * half_x : (g + 1) * half_x].astype(F32), axis=0)
            for g in range(KV_HEADS)
        ]
        dk = jnp.concatenate([s[:, 0:HEAD_DIM] * factor for s in sums], axis=1).astype(BF16)
        dv = jnp.concatenate([s[:, HEAD_DIM:] for s in sums], axis=1).astype(BF16)
        sg_v[...] = dot(dk, kw_v[...], NT) + dot(dv, vw_v[...], NT)
        put_sg.start()

    def target_out():
        for o in near:
            arrive(f_r.at[chip(-o)], recvs["f", o])
        grad = jnp.sum(f_r[...].astype(F32), axis=0)
        wide = t_v[...].astype(F32)
        root = jnp.sqrt(jnp.mean(wide * wide, axis=1, keepdims=True) + 1e-06)
        scaled = grad * gain_v[...]
        mean = jnp.mean(scaled * wide, axis=1, keepdims=True)
        tg_v[...] = scaled / root - wide * mean / (root * root * root)
        put_tg.start()

    def rest(stage):
        if stage == 0:
            row_share()
        if stage == 1:
            source_out()
        if stage == 3:
            target_out()

    def own_g(b, cut):
        return gp[b, cut]

    wg_v[...] = ring_sum("g", own_g, g_snd, g_raw, g_sum, rest).T
    put_wg.start()
    for copy in started:
        copy.wait_send()
    for copy in c_copies:
        copy.wait_send()

    @pl.when(c == 1)
    def _():
        for copy in st_copies:
            copy.wait_send()
        mate_stat.wait_send()

    @pl.when(c == 0)
    def _():
        mate_rows.wait_send()

    put_sg.wait()
    put_tg.wait()
    put_wg.wait()


def shards(
    target, source, norm_gain, query_weight, key_weight, value_weight, output_weight, saved_out,
    log_shift, out_grad,
):
    n, m = lax.axis_size("sp"), lax.axis_size("tp")
    rows, width = target.shape
    srows = source.shape[0]
    chips, tgt, src = m // 2, rows * m, srows * m
    cols = width // n
    half = n // 2 + 1
    hd = HEAD_DIM
    vmem = pltpu.VMEM
    scratch = [
        vmem((rows, width), BF16),
        vmem((srows, width), BF16),
        vmem((1, width), F32),
        vmem((width, 2 * hd), BF16),
        vmem((width, KV_HEADS * hd), BF16),
        vmem((width, KV_HEADS * hd), BF16),
        vmem((2 * hd, width), BF16),
        vmem((2, tgt, hd), BF16),
        vmem((2, 1, tgt), F32),
        vmem((2, rows, width), BF16),
        vmem((m, rows, width), BF16),
        vmem((tgt, width), BF16),
        vmem((tgt, width), BF16),
        vmem((KV_HEADS, srows, 2 * hd), BF16),
        vmem((m, srows, 2 * hd), BF16),
        vmem((hd, src), BF16),
        vmem((n, 2 * tgt, 2 * hd), BF16),
        vmem((2, tgt, hd), BF16),
        vmem((2, 2, tgt), F32),
        vmem((n, 2, tgt), F32),
        vmem((chips, 2, srows, 2 * hd), F32),
        vmem((n, hd, tgt), F32),
        vmem((n, hd, cols), F32),
        *[vmem((2, half, hd, tgt), BF16)] * 3,
        *[vmem((2, half, hd, cols), BF16)] * 3,
        *[vmem((chips, srows, 2 * hd), BF16)] * 4,
        vmem((2, chips, rows, hd), BF16),
        vmem((chips, rows, hd), BF16),
        *[vmem((chips, rows, width), BF16)] * 2,
        vmem((rows, width), F32),
        vmem((srows, width), F32),
        vmem((cols, hd), F32),
        pltpu.SemaphoreType.DMA((16,)),
        pltpu.SemaphoreType.DMA((400,)),
        pltpu.SemaphoreType.DMA((400,)),
        pltpu.SemaphoreType.DMA((2, C_SUBS, 2)),
        pltpu.SemaphoreType.DMA((2, half, 2, C_SUBS)),
        pltpu.SemaphoreType.DMA((3, 2)),
    ]
    anywhere = pl.BlockSpec(memory_space=pl.ANY)
    return pl.pallas_call(
        functools.partial(kernel, (n, m, rows, srows, width)),
        out_shape=(
            jax.ShapeDtypeStruct((rows, width), F32),
            jax.ShapeDtypeStruct((srows, width), F32),
            jax.ShapeDtypeStruct((cols, hd), F32),
        ),
        in_specs=[anywhere] * 10,
        out_specs=(anywhere,) * 3,
        scratch_shapes=scratch,
        compiler_params=pltpu.CompilerParams(
            collective_id=0, has_side_effects=True, vmem_limit_bytes=48 * 1024 * 1024
        ),
    )(
        target, source, norm_gain.reshape(1, width), query_weight, key_weight, value_weight,
        output_weight, saved_out, log_shift, out_grad,
    )


def solution(mesh):
    return jax.shard_map(
        shards,
        mesh=mesh,
        in_specs=(
            P(("grp", "sp", "tp"), None),
            P(("grp", "sp", "tp"), None),
            P(),
            P(None, "tp"),
            P(),
            P(),
            P("tp", None),
            P(("grp", "sp"), "tp"),
            P("tp", ("grp", "sp")),
            P(("grp", "sp", "tp"), None),
        ),
        out_specs=(
            P(("grp", "sp", "tp"), None),
            P(("grp", "sp", "tp"), None),
            P(("grp", "sp"), "tp"),
        ),
        check_vma=False,
    )
```

```python
import functools
import math

import jax
import jax.numpy as jnp
from jax import lax
from jax.experimental import pallas as pl
from jax.experimental.pallas import tpu as pltpu
from jax.sharding import PartitionSpec as P

HEAD_DIM = 128
KV_HEADS = 2
A_SUBS = 2
C_SUBS = 2
R_SUBS = 2
TILE = 512
LOG2E = math.log2(math.e)
F32, BF16 = jnp.float32, jnp.bfloat16
NT = (((1,), (1,)), ((), ()))


def dot(a, b, dims=(((1,), (0,)), ((), ()))):
    return lax.dot_general(a, b, dims, preferred_element_type=F32)


class Sems:
    def __init__(self, ref):
        self.ref, self.names = ref, {}

    def __getitem__(self, name):
        index = self.names.setdefault(name, len(self.names))
        assert index < self.ref.shape[0], index
        return self.ref.at[index]


def size_of(ref):
    return math.prod(ref.shape) * jnp.dtype(ref.dtype).itemsize


def kernel(sizes, *refs):
    n, m, rows, srows, width = sizes
    chips, half_n, half_x = m // 2, n // 2, m // 4
    tgt, src = rows * m, srows * m
    (t_h, s_h, gain_h, wq_h, kw_h, vw_h, wo_h, saved_h, shift_h, og_h) = refs[:10]
    (tg_h, sg_h, wg_h) = refs[10:13]
    (
        t_v, s_v, gain_v, wq2, kw_v, vw_v, wo2, saved2, shift2,
        kinds, rows_all, rows_mat, nrm_mat, kvs, kv_all, k_t, blk, stg, stat_s, stat,
        acc, dqp, gp, d_snd, d_raw, d_sum, g_snd, g_raw, g_sum,
        pk_s, pk_r, ek_s, ek_r, dq_s, dq_r, f_s, f_r, tg_v, sg_v, wg_v,
        ruler, load_ref, send_ref, recv_ref,
    ) = refs[13:]
    tp, sp = lax.axis_index("tp"), lax.axis_index("sp")
    x, c = tp // 2, tp % 2
    mate = x * 2 + 1 - c

    def chip(o):
        return (x + o + chips) % chips

    def ring(o):
        return (sp + o + n) % n

    loads, sends, recvs = Sems(load_ref), Sems(send_ref), Sems(recv_ref)
    sent = {}

    def remote(source, target, group, name, device):
        return pltpu.make_async_remote_copy(
            src_ref=source, dst_ref=target, send_sem=sends[group], recv_sem=recvs[name],
            device_id=device, device_id_type=pl.DeviceIdType.MESH,
        )

    def load(source, target, name):
        copy = pltpu.make_async_copy(source, target, loads[name])
        copy.start()
        return copy

    def send(source, target, group, name, device):
        remote(source, target, group, name, device).start()
        sent[group] = sent.get(group, 0) + size_of(source)

    def arrive(target, *name):
        remote(target, target, "a", name, {"tp": mate}).wait_recv()

    def length(size):
        return ruler.at[pl.ds(0, size // (2 * 128 * 4))]

    get_t = load(t_h, t_v, "t")
    get_gain = load(gain_h, gain_v, "gain")
    get_og = load(og_h, kinds.at[1], "og")
    get_s = load(s_h, s_v, "s")
    get_kw = load(kw_h, kw_v, "kw")
    get_vw = load(vw_h, vw_v, "vw")
    get_wq = load(wq_h, wq2.at[:, 0:HEAD_DIM], "wq")
    get_wo = load(wo_h, wo2.at[0:HEAD_DIM], "wo")
    get_saved = load(saved_h, saved2.at[0], "saved")
    get_shift = load(shift_h, shift2.at[0], "shift")

    peers = [{"tp": chip(o) * 2 + c} for o in range(1, chips)]
    peers += [{"tp": chip(o) * 2 + 1 - c} for o in (-2, -1, 0, 1, 2)]
    peers += [{"sp": ring(o), "tp": j} for o in (-2, -1, 1, 2) for j in (tp, mate)]
    barrier = pltpu.get_barrier_semaphore()
    for peer in peers:
        pl.semaphore_signal(barrier, inc=1, device_id=peer, device_id_type=pl.DeviceIdType.MESH)

    get_t.wait()
    get_gain.wait()
    wide = t_v[...].astype(F32)
    root = jnp.sqrt(jnp.mean(wide * wide, axis=1, keepdims=True) + 1e-06)
    kinds[0] = (wide / root * gain_v[...]).astype(BF16)
    get_og.wait()
    rows_all[tp] = kinds[c]
    pl.semaphore_wait(barrier, len(peers))

    half_x_ring = chips // 2
    part = width // A_SUBS
    cuts = [pl.ds(i * part, part) for i in range(A_SUBS)]

    def a_far(way, i):
        return half_x_ring - ((i < A_SUBS // 2) != (way == 1))

    for i, cut in enumerate(cuts):
        for d in (2, 1):
            for way in (1, -1):
                if d <= a_far(way, i):
                    for k in (0, 1):
                        send(
                            kinds.at[k, :, cut], rows_all.at[tp, :, cut], "a", ("a", way, d, i),
                            {"tp": chip(way * d) * 2 + k},
                        )
    send(kinds.at[1 - c], rows_all.at[tp], "a", ("mate_rows",), {"tp": mate})
    send(wq_h, wq2.at[:, HEAD_DIM : 2 * HEAD_DIM], "wq", ("wq",), {"tp": mate})
    send(wo_h, wo2.at[HEAD_DIM : 2 * HEAD_DIM], "wo", ("wo",), {"tp": mate})
    send(saved_h, saved2.at[1], "saved", ("saved",), {"tp": mate})
    send(shift_h, shift2.at[1], "shift", ("shift",), {"tp": mate})

    get_s.wait()
    get_kw.wait()
    get_vw.wait()
    keys = dot(s_v[...], kw_v[...]).astype(BF16)
    values = dot(s_v[...], vw_v[...]).astype(BF16)
    for g in range(KV_HEADS):
        piece = slice(g * HEAD_DIM, (g + 1) * HEAD_DIM)
        kvs[g, :, 0:HEAD_DIM] = keys[:, piece]
        kvs[g, :, HEAD_DIM:] = values[:, piece]

    near = [o for k in range(1, half_x_ring + 1) for o in (k, -k)][: chips - 1]
    for d in range(2, half_x_ring + 2, 2):
        for i, cut in enumerate(cuts):
            for way in (1, -1):
                if d > a_far(way, i):
                    continue
                piece = rows_all.at[pl.ds(chip(-way * d) * 2, 2), :, cut]
                arrive(piece, "a", way, d, i)
                for more in (2, 1):
                    if d + more <= a_far(way, i):
                        send(
                            piece, piece, "a", ("a", way, d + more, i),
                            {"tp": chip(way * more) * 2 + c},
                        )
        if d == 2:
            for o in near[::-1]:
                to = chip(o)
                send(kvs.at[to // half_x], kv_all.at[tp], "kv", ("kv", o), {"tp": to * 2 + c})
            kv_all[tp] = kvs[x // half_x]
            blk[:, 0:tgt, HEAD_DIM:] = jnp.zeros((n, tgt, HEAD_DIM), BF16)
            blk[:, tgt:, 0:HEAD_DIM] = jnp.zeros((n, tgt, HEAD_DIM), BF16)
            acc[...] = jnp.zeros(acc.shape, F32)
    for d in range(1, half_x_ring + 1, 2):
        for i, cut in enumerate(cuts):
            for way in (1, -1):
                if d <= a_far(way, i):
                    arrive(rows_all.at[pl.ds(chip(-way * d) * 2, 2), :, cut], "a", way, d, i)
    arrive(rows_all.at[tp], "mate_rows")
    rows_mat[...] = rows_all[...].astype(F32).reshape(tgt, width).astype(BF16)
    get_wq.wait()
    get_wo.wait()
    get_saved.wait()
    get_shift.wait()
    for name, target in (
        ("wq", wq2.at[:, HEAD_DIM : 2 * HEAD_DIM]), ("wo", wo2.at[HEAD_DIM : 2 * HEAD_DIM]),
        ("saved", saved2.at[1]), ("shift", shift2.at[1]),
    ):
        arrive(target, name)

    offset = math.log(n * src)

    @pl.when(c == 0)
    def _():
        both = dot(rows_mat[...], wq2[...]).astype(BF16)
        stg[0] = both[:, 0:HEAD_DIM]
        stg[1] = both[:, HEAD_DIM:]

    @pl.when(c == 1)
    def _():
        both = dot(rows_mat[...], wo2[...], NT).astype(BF16)
        stg[0] = both[:, 0:HEAD_DIM]
        stg[1] = both[:, HEAD_DIM:]
        for k in (0, 1):
            product = stg[k].astype(F32) * saved2[k].astype(F32)
            stat_s[k, 0:1, :] = (shift2[k] + offset) * LOG2E
            stat_s[k, 1:2, :] = jnp.sum(product.T, axis=0, keepdims=True)
        stat[sp] = stat_s[0]

    piece_rows = tgt // C_SUBS

    def c_piece(b, kind, i):
        return blk.at[
            b, pl.ds(kind * tgt + i * piece_rows, piece_rows), pl.ds(kind * HEAD_DIM, HEAD_DIM)
        ]


    def c_far(way, kind):
        return half_n - ((kind == 0) != (way == 1))

    mine = pl.multiple_of(c * tgt, tgt)
    lane = pl.multiple_of(c * HEAD_DIM, HEAD_DIM)
    own_lane = pl.ds(lane, HEAD_DIM)
    for i in range(C_SUBS):
        own_rows = pl.ds(pl.multiple_of(mine + i * piece_rows, piece_rows), piece_rows)
        for d in (2, 1):
            for way in (1, -1):
                for k in (0, 1):
                    send(
                        stg.at[k, pl.ds(i * piece_rows, piece_rows)],
                        blk.at[sp, own_rows, own_lane], "c", ("c", way, d, i),
                        {"sp": ring(way * d), "tp": tp if k == 0 else mate},
                    )
    own_stats = [
        remote(
            stat_s.at[k], stat.at[sp], "own_stat", ("stat", way, d),
            {"sp": ring(way * d), "tp": tp if k == 0 else mate},
        )
        for d in (2, 1) for way in (1, -1) for k in (0, 1)
    ]
    mate_stat = remote(stat_s.at[1], stat.at[sp], "mate_stat", ("mate_stat",), {"tp": mate})
    mate_rows = remote(rows_mat, nrm_mat, "nrm", ("nrm",), {"tp": mate})
    send(stg.at[1], blk.at[sp, pl.ds(mine, tgt), own_lane], "c", ("mate_block",), {"tp": mate})
    blk[sp, pl.ds(mine, tgt), own_lane] = stg[0]

    @pl.when(c == 1)
    def _():
        for copy in own_stats:
            copy.start()
        mate_stat.start()

    @pl.when(c == 0)
    def _():
        mate_rows.start()
        nrm_mat[...] = rows_mat[...]

    def c_arrive(way, d, i):
        b = ring(-way * d)
        kinds_here = [kind for kind in (0, 1) if d <= c_far(way, kind)]
        rows_here = len(kinds_here) * piece_rows
        arrive(blk.at[b, pl.ds(0, rows_here), pl.ds(0, HEAD_DIM)], "c", way, d, i)
        return b, kinds_here

    def c_even(d):
        for i in range(C_SUBS):
            for way in (1, -1):
                b, kinds_here = c_arrive(way, d, i)
                for more in (2, 1):
                    for kind in kinds_here:
                        if d + more <= c_far(way, kind):
                            piece = c_piece(b, kind, i)
                            send(
                                piece, piece, "c", ("c", way, d + more, i),
                                {"sp": ring(way * more)},
                            )
        for way in (1, -1):
            if d <= c_far(way, 0):
                piece = stat.at[ring(-way * d)]
                arrive(piece, "stat", way, d)
                for more in (2, 1):
                    if d + more <= c_far(way, 0):
                        send(piece, piece, "stat", ("stat", way, d + more), {"sp": ring(way * more)})

    def c_odd(d):
        for way in (1, -1):
            for i in range(C_SUBS):
                c_arrive(way, d, i)
            arrive(stat.at[ring(-way * d)], "stat", way, d)

    def kv_pass():
        for o in [0] + near:
            slot = kv_all.at[chip(-o) * 2 + c]
            if o != 0:
                arrive(slot, "kv", o)
            send(slot, slot, "kv", ("kv_mate",), {"tp": mate})

    def kv_ready():
        arrive(kv_all.at[pl.ds(0, chips)], "kv_mate")
        k_t[...] = kv_all[:, :, 0:HEAD_DIM].reshape(src, HEAD_DIM).T

        @pl.when(c == 0)
        def _():
            arrive(c_own(1), "mate_block")
            arrive(stat.at[sp], "mate_stat")

        @pl.when(c == 1)
        def _():
            arrive(c_own(0), "mate_block")

    def c_own(kind):
        return blk.at[sp, kind * tgt : (kind + 1) * tgt, kind * HEAD_DIM : (kind + 1) * HEAD_DIM]

    factor = HEAD_DIM ** (-0.5)
    tile = min(TILE, src)
    step = tile // srows

    def attend(index, carry):
        away = (index + 1) // 2 * (1 - 2 * (index % 2))
        b = (sp + away + n) % n
        block = blk[b]
        stats = stat[b]
        total = jnp.zeros((HEAD_DIM, tgt), F32)
        for at in range(0, m, step):
            kv = kv_all[at : at + step].reshape(tile, 2 * HEAD_DIM)
            both = dot(kv, block, NT)
            prob = jnp.exp2(both[:, 0:tgt] * (factor * LOG2E) - stats[0:1])
            grad = (prob * (both[:, tgt:] - stats[1:2])).astype(BF16)
            pair = jnp.concatenate([grad, prob.astype(BF16)], axis=1)
            added = dot(pair, block).reshape(step // 2, 2, srows, 2 * HEAD_DIM)
            acc[at // 2 : (at + step) // 2] += added
            total += dot(k_t[:, at * srows : at * srows + tile], grad)
        dqp[b] = total
        return carry

    done = 0
    kv_pass()
    for d in range(2, half_n + 2, 2):
        c_even(d)
        if d == 2:
            kv_ready()
        c_odd(d - 1)
        upto = n if d == half_n else min(done + 4, 1 + 2 * d)
        lax.fori_loop(done, upto, attend, 0)
        done = upto

    def ring_sum(name, own, snd, raw, total, between):
        chunk = HEAD_DIM // R_SUBS
        limits = (half_n, half_n - 1)
        order = []
        for d in range(half_n, 0, -1):
            for side in (0, 1):
                if d <= limits[side]:
                    order.append((side, d))

        def block(side, d):
            return ring(-d if side == 0 else d)

        def put(side, d, i):
            cut = pl.ds(i * chunk, chunk)
            back = -1 if side == 0 else 1
            into = raw if d % 2 else total
            send(
                snd.at[side, d, cut], into.at[side, d, cut], name,
                (name, side, (d - 1) // 2, i), {"sp": ring(back if d % 2 else 2 * back)},
            )

        def term(side, d, i, value):
            cut = pl.ds(i * chunk, chunk)
            arrive(raw.at[side, pl.ds(0, 1 + (d + 2 <= limits[side])), cut], name, side, d // 2, i)
            value += raw[side, d + 1, cut].astype(F32)
            if d + 2 <= limits[side]:
                value += total[side, d + 2, cut].astype(F32)
            return value

        for side, d in order:
            if d % 2 or d == half_n:
                snd[side, d] = own(block(side, d), slice(None)).astype(BF16)
                for i in range(R_SUBS):
                    put(side, d, i)
        between(0)
        for stage, d in enumerate(range(half_n - 2, 0, -2)):
            if stage:
                between(stage)
            for i in range(R_SUBS):
                for side in (0, 1):
                    cut = pl.ds(i * chunk, chunk)
                    snd[side, d, cut] = term(side, d, i, own(block(side, d), cut)).astype(BF16)
                    put(side, d, i)
        for stage in range(max(1, half_n // 2 - 1), 4):
            between(stage)
        parts = []
        for i in range(R_SUBS):
            value = own(sp, pl.ds(i * chunk, chunk))
            for side in (0, 1):
                value = term(side, 0, i, value)
            parts.append(value)
        return jnp.concatenate(parts, axis=0)

    def own_dq(b, cut):
        return dqp[b, cut]

    def kv_pair(stage):
        if stage == 0:
            pk_s[...] = acc[:, 1 - c].astype(BF16)
            send(pk_s, pk_r, "pk", ("pk",), {"tp": mate})
        if stage == 1:
            arrive(pk_r, "pk")
            ek_s[...] = (acc[:, c] + pk_r[...].astype(F32)).astype(BF16)
            for o in near[::-1]:
                send(ek_s.at[chip(o)], ek_r.at[x], "ek", ("ek",), {"tp": chip(o) * 2 + c})
            ek_r[x] = ek_s[x]

    dq_t = (ring_sum("d", own_dq, d_snd, d_raw, d_sum, kv_pair) * factor).astype(BF16)

    dq_rows = dq_t.astype(F32).T.reshape(chips, 2, rows, HEAD_DIM)
    dq_s[0] = dq_rows[:, 0].astype(BF16)
    dq_s[1] = dq_rows[:, 1].astype(BF16)
    send(dq_s.at[1 - c], dq_r, "dq", ("dq",), {"tp": mate})

    @pl.when(c == 1)
    def _():
        arrive(nrm_mat, "nrm")

    shares = dot(dq_t, nrm_mat[...])
    cols = width // n
    for b in range(n):
        gp[b] = shares[:, b * cols : (b + 1) * cols]

    def row_share():
        arrive(dq_r, "dq")
        left = dq_s[c].astype(F32).reshape(chips * rows, HEAD_DIM).astype(BF16)
        right = dq_r[...].astype(F32).reshape(chips * rows, HEAD_DIM).astype(BF16)
        share = dot(jnp.concatenate([left, right], axis=1), wq2[...], NT)
        f_s[...] = share.reshape(chips, rows, width).astype(BF16)
        for o in near[::-1]:
            send(f_s.at[chip(o)], f_r.at[x], "f", ("f",), {"tp": chip(o) * 2 + c})
        f_r[x] = f_s[x]

    put_sg = pltpu.make_async_copy(sg_v, sg_h, loads["sg"])
    put_tg = pltpu.make_async_copy(tg_v, tg_h, loads["tg"])
    put_wg = pltpu.make_async_copy(wg_v, wg_h, loads["wg"])

    def source_out():
        arrive(ek_r.at[pl.ds(0, chips - 1)], "ek")
        sums = [
            jnp.sum(ek_r[g * half_x : (g + 1) * half_x].astype(F32), axis=0)
            for g in range(KV_HEADS)
        ]
        dk = jnp.concatenate([s[:, 0:HEAD_DIM] * factor for s in sums], axis=1).astype(BF16)
        dv = jnp.concatenate([s[:, HEAD_DIM:] for s in sums], axis=1).astype(BF16)
        sg_v[...] = dot(dk, kw_v[...], NT) + dot(dv, vw_v[...], NT)
        put_sg.start()

    def target_out():
        arrive(f_r.at[pl.ds(0, chips - 1)], "f")
        grad = jnp.sum(f_r[...].astype(F32), axis=0)
        wide = t_v[...].astype(F32)
        root = jnp.sqrt(jnp.mean(wide * wide, axis=1, keepdims=True) + 1e-06)
        scaled = grad * gain_v[...]
        mean = jnp.mean(scaled * wide, axis=1, keepdims=True)
        tg_v[...] = scaled / root - wide * mean / (root * root * root)
        put_tg.start()

    def rest(stage):
        if stage == 1:
            row_share()
        if stage == 2:
            source_out()
        if stage == 3:
            target_out()

    def own_g(b, cut):
        return gp[b, cut]

    wg_v[...] = ring_sum("g", own_g, g_snd, g_raw, g_sum, rest).T
    put_wg.start()
    sources = {"wq": wq_h, "wo": wo_h, "saved": saved_h, "shift": shift_h}
    for group, size in sent.items():
        whole = sources.get(group) if group in sources else length(size)
        remote(whole, whole, group, ("pk",), {"tp": mate}).wait_send()

    @pl.when(c == 1)
    def _():
        whole = length(len(own_stats) * size_of(stat_s.at[0]))
        remote(whole, whole, "own_stat", ("pk",), {"tp": mate}).wait_send()
        mate_stat.wait_send()

    @pl.when(c == 0)
    def _():
        mate_rows.wait_send()

    put_sg.wait()
    put_tg.wait()
    put_wg.wait()


def shards(
    target, source, norm_gain, query_weight, key_weight, value_weight, output_weight, saved_out,
    log_shift, out_grad,
):
    n, m = lax.axis_size("sp"), lax.axis_size("tp")
    rows, width = target.shape
    srows = source.shape[0]
    chips, tgt, src = m // 2, rows * m, srows * m
    cols = width // n
    half = n // 2 + 1
    hd = HEAD_DIM
    vmem = pltpu.VMEM
    scratch = [
        vmem((rows, width), BF16),
        vmem((srows, width), BF16),
        vmem((1, width), F32),
        vmem((width, 2 * hd), BF16),
        vmem((width, KV_HEADS * hd), BF16),
        vmem((width, KV_HEADS * hd), BF16),
        vmem((2 * hd, width), BF16),
        vmem((2, tgt, hd), BF16),
        vmem((2, 1, tgt), F32),
        vmem((2, rows, width), BF16),
        vmem((m, rows, width), BF16),
        vmem((tgt, width), BF16),
        vmem((tgt, width), BF16),
        vmem((KV_HEADS, srows, 2 * hd), BF16),
        vmem((m, srows, 2 * hd), BF16),
        vmem((hd, src), BF16),
        vmem((n, 2 * tgt, 2 * hd), BF16),
        vmem((2, tgt, hd), BF16),
        vmem((2, 2, tgt), F32),
        vmem((n, 2, tgt), F32),
        vmem((chips, 2, srows, 2 * hd), F32),
        vmem((n, hd, tgt), F32),
        vmem((n, hd, cols), F32),
        *[vmem((2, half, hd, tgt), BF16)] * 3,
        *[vmem((2, half, hd, cols), BF16)] * 3,
        *[vmem((chips, srows, 2 * hd), BF16)] * 4,
        vmem((2, chips, rows, hd), BF16),
        vmem((chips, rows, hd), BF16),
        *[vmem((chips, rows, width), BF16)] * 2,
        vmem((rows, width), F32),
        vmem((srows, width), F32),
        vmem((cols, hd), F32),
        vmem((1024, 2, 128), F32),
        pltpu.SemaphoreType.DMA((13,)),
        pltpu.SemaphoreType.DMA((17,)),
        pltpu.SemaphoreType.DMA((113,)),
    ]
    anywhere = pl.BlockSpec(memory_space=pl.ANY)
    return pl.pallas_call(
        functools.partial(kernel, (n, m, rows, srows, width)),
        out_shape=(
            jax.ShapeDtypeStruct((rows, width), F32),
            jax.ShapeDtypeStruct((srows, width), F32),
            jax.ShapeDtypeStruct((cols, hd), F32),
        ),
        in_specs=[anywhere] * 10,
        out_specs=(anywhere,) * 3,
        scratch_shapes=scratch,
        compiler_params=pltpu.CompilerParams(
            collective_id=0, has_side_effects=True, vmem_limit_bytes=64_000_000
        ),
    )(
        target, source, norm_gain.reshape(1, width), query_weight, key_weight, value_weight,
        output_weight, saved_out, log_shift, out_grad,
    )


def solution(mesh):
    return jax.shard_map(
        shards,
        mesh=mesh,
        in_specs=(
            P(("grp", "sp", "tp"), None),
            P(("grp", "sp", "tp"), None),
            P(),
            P(None, "tp"),
            P(),
            P(),
            P("tp", None),
            P(("grp", "sp"), "tp"),
            P("tp", ("grp", "sp")),
            P(("grp", "sp", "tp"), None),
        ),
        out_specs=(
            P(("grp", "sp", "tp"), None),
            P(("grp", "sp", "tp"), None),
            P(("grp", "sp"), "tp"),
        ),
        check_vma=False,
    )
```
